32 devices in a mesh: ep: 4 (over y, x), tp: 8 (over z, core).
Axes of the slice: x: 2, y: 2, z: 4, core: 2. Of those that a mesh axis runs over, the one named last changes fastest.
Arguments:
- hidden: bfloat16 [160, 4096], P('ep', 'tp'), may hold values from -6 to 6
- positions: int32 [160], P('ep'), may hold values from 0 to 16383
- ret_state: float32 [160, 16, 128, 128], P('ep', 'tp'), may hold values from -1.5 to 1.5
- query_weight: bfloat16 [4096, 2048], P('ep', 'tp'), may hold values from -0.09375 to 0.09375
- key_weight: bfloat16 [4096, 2048], P('ep', 'tp'), may hold values from -0.09375 to 0.09375
- value_weight: bfloat16 [4096, 2048], P('ep', 'tp'), may hold values from -0.09375 to 0.09375
- gate_weight: bfloat16 [4096, 2048], P('ep', 'tp'), may hold values from -0.09375 to 0.09375
- head_gain: float32 [2048], P('tp'), may hold values from 0.1 to 1.9
- out_weight: bfloat16 [2048, 4096], P(None, 'tp'), may hold values from -0.125 to 0.125
- mix_gain: float32 [4096], replicated, may hold values from 0.1 to 1.9
- ffn_gain: float32 [4096], replicated, may hold values from 0.1 to 1.9
- expert_gate: bfloat16 [8, 4096, 2048], P('ep', None, 'tp'), may hold values from -0.09375 to 0.09375
- expert_up: bfloat16 [8, 4096, 2048], P('ep', None, 'tp'), may hold values from -0.09375 to 0.09375
- expert_down: bfloat16 [8, 2048, 4096], P('ep', None, 'tp'), may hold values from -0.125 to 0.125
- route_ids: int32 [160, 2], P('ep'), may hold values from 0 to 7, as said below
- route_weight: float32 [160, 2], P('ep'), may hold values from 0.25 to 1
Outputs:
- updated: bfloat16 [160, 4096], P('ep', 'tp')
- next_state: float32 [160, 16, 128, 128], P('ep', 'tp')
The draws below stay inside these ranges and needn't reach their ends.
Inputs may be any that keep to these rules, and one draw needn't show every extreme that they name: `route_ids`: each row names two different experts of one group, the group being the numbers g * 2 to g * 2 + 1; in the rows of one device (aligned blocks of 40 rows) no expert is named more than 10 times, and some expert is named exactly 10 times.
All inputs are finite; a program needn't handle non-finite values.
Results may differ from the reference program's by a relative error of at most 0.014.
Values may be sent and summed in bfloat16 or wider, within the bound.
A program may use at most 64 MiB of HBM per device.

```python
import jax
import jax.numpy as jnp
from jax import lax

D = 4096
HEADS = 16
HEAD = 128
RD = 2048
FF = 2048
GROUPS = 4
EXPERTS = 8
TOP = 2
B_DEV = 40
BATCH = 160
CAP = 10
MAXPOS = 16384
N_EP = 4


def draw_route_ids(key, part):
    blocks = BATCH // B_DEV
    group_size = EXPERTS // GROUPS
    order_key, shift_key = jax.random.split(key)
    orders = jax.vmap(lambda item: jax.random.permutation(item, B_DEV))(jax.random.split(order_key, blocks))
    shifts = jax.random.randint(shift_key, (blocks, GROUPS), 0, group_size)
    group = orders % GROUPS
    within = orders // GROUPS
    offset = jnp.take_along_axis(shifts, group, axis=1)
    first = (within + offset) % group_size
    second = (first + 1) % group_size
    pairs = jnp.stack([group * group_size + first, group * group_size + second], axis=-1)
    return pairs.reshape(BATCH, TOP).astype(jnp.int32)


def place_ends(values, key, least, largest):
    spot = [jax.random.randint(jax.random.fold_in(key, axis), (), 0, length) for axis, length in enumerate(values.shape)]
    longest = values.shape.index(max(values.shape))
    beside = spot[:longest] + [(spot[longest] + 1) % values.shape[longest]] + spot[longest + 1:]
    return values.at[tuple(spot)].set(least).at[tuple(beside)].set(largest)


def block_levels(own_key, extent, shards, low, largest):
    def one(axis_at, blocks):
        draws = jax.random.uniform(jax.random.fold_in(jax.random.fold_in(own_key, 6), axis_at), (blocks,), jnp.float32, low / len(shards), largest / len(shards))
        return jnp.repeat(jnp.exp(draws), extent[axis_at] // blocks).reshape((-1,) + (1,) * (len(extent) - axis_at - 1))

    level = one(*shards[0])
    for cut in shards[1:]:
        level = level * one(*cut)
    return level


def scatter_about(rng, dims, scale, bound, cuts=(), held_as=jnp.bfloat16):
    values = scale * jax.random.normal(rng, dims, jnp.float32)
    if cuts:
        values = values * block_levels(rng, dims, cuts, -0.22, 0.18)
    return jnp.clip(values, -bound, bound).astype(held_as)


def setup_inputs(seed: int = 0) -> dict:
    keys = jax.random.split(jax.random.key(seed), 17)
    hidden = scatter_about(keys[0], (BATCH, D), 1.0, 6.0, ((0, 4), (1, 8)))
    positions = place_ends(jax.random.randint(keys[1], (BATCH,), 0, MAXPOS), jax.random.fold_in(keys[1], 1), 0, MAXPOS - 1).astype(jnp.int32)
    ret_state = scatter_about(keys[2], (BATCH, HEADS, HEAD, HEAD), 0.25, 1.5, ((0, 4), (1, 8)), jnp.float32)
    query_weight = scatter_about(keys[3], (D, RD), D ** -0.5, 0.09375, ((0, 4), (1, 8)))
    key_weight = scatter_about(keys[4], (D, RD), D ** -0.5, 0.09375, ((0, 4), (1, 8)))
    value_weight = scatter_about(keys[5], (D, RD), D ** -0.5, 0.09375, ((0, 4), (1, 8)))
    gate_weight = scatter_about(keys[6], (D, RD), D ** -0.5, 0.09375, ((0, 4), (1, 8)))
    head_gain = jnp.clip(1.0 + 0.18 * jax.random.normal(keys[7], (RD,), jnp.float32), 0.1, 1.9)
    out_weight = scatter_about(keys[8], (RD, D), RD ** -0.5, 0.125, ((1, 8),))
    mix_gain = jnp.clip(1.0 + 0.18 * jax.random.normal(keys[9], (D,), jnp.float32), 0.1, 1.9)
    ffn_gain = jnp.clip(1.0 + 0.18 * jax.random.normal(keys[10], (D,), jnp.float32), 0.1, 1.9)
    expert_gate = scatter_about(keys[11], (EXPERTS, D, FF), D ** -0.5, 0.09375, ((0, 4), (2, 8)))
    expert_up = scatter_about(keys[12], (EXPERTS, D, FF), D ** -0.5, 0.09375, ((0, 4), (2, 8)))
    expert_down = scatter_about(keys[13], (EXPERTS, FF, D), FF ** -0.5, 0.125, ((0, 4), (2, 8)))
    route_ids = draw_route_ids(jax.random.fold_in(keys[16], 71), 0)
    route_weight = jnp.clip(0.25 + 0.75 * jax.random.uniform(keys[15], (BATCH, TOP), jnp.float32) ** block_levels(keys[15], (BATCH, TOP), ((0, 4),), -0.2, 0.2), 0.25, 1.0)
    return dict(hidden=hidden, positions=positions, ret_state=ret_state, query_weight=query_weight, key_weight=key_weight, value_weight=value_weight, gate_weight=gate_weight, head_gain=head_gain, out_weight=out_weight, mix_gain=mix_gain, ffn_gain=ffn_gain, expert_gate=expert_gate, expert_up=expert_up, expert_down=expert_down, route_ids=route_ids, route_weight=route_weight)


epsilon = 1e-06
rope_base = 10000.0

def rms_scale(rows, gain):
    values = rows.astype(jnp.float32)
    factor = lax.rsqrt(lax.optimization_barrier(jnp.mean(values * values, axis=-1, keepdims=True)) + epsilon)
    return (values * factor * gain).astype(jnp.bfloat16)

def log_decay(head_ids):
    return jnp.log(1.0 - 2.0 ** (-5.0 - 5.0 * head_ids.astype(jnp.float32) / (HEADS - 1)))

def rotate(values, positions):
    width = values.shape[-1]
    inverse = 1.0 / rope_base ** (jnp.arange(0, width, 2, dtype=jnp.float32) / width)
    angle = positions.astype(jnp.float32)[:, None, None] * inverse[None, None, :]
    cosine = jnp.cos(angle)
    sine = jnp.sin(angle)
    first = values[..., :width // 2]
    second = values[..., width // 2:]
    return jnp.concatenate([first * cosine - second * sine, first * sine + second * cosine], axis=-1)

def retain(query, key_rows, value_rows, gate_rows, ret_state, positions, head_ids, head_gain):
    batch = query.shape[0]
    heads = head_ids.shape[0]

    def split(array):
        return array.astype(jnp.float32).reshape(batch, heads, HEAD)
    rotated_query = rotate(split(query), positions)
    rotated_key = rotate(split(key_rows), positions) * HEAD ** (-0.5)
    value_heads = split(value_rows)
    decay = jnp.exp(log_decay(head_ids))
    next_state = decay[None, :, None, None] * ret_state + rotated_key[..., :, None] * value_heads[..., None, :]
    read = jnp.einsum('bhd,bhde->bhe', rotated_query, next_state, precision=lax.Precision.HIGHEST)
    centered = read - lax.optimization_barrier(jnp.mean(read, axis=-1, keepdims=True))
    normal = centered * lax.rsqrt(lax.optimization_barrier(jnp.mean(centered * centered, axis=-1, keepdims=True)) + epsilon)
    mixed = normal.reshape(batch, heads * HEAD) * head_gain * jax.nn.silu(gate_rows.astype(jnp.float32))
    return (mixed.astype(jnp.bfloat16), next_state)

def reference(hidden, positions, ret_state, query_weight, key_weight, value_weight, gate_weight, head_gain, out_weight, mix_gain, ffn_gain, expert_gate, expert_up, expert_down, route_ids, route_weight):
    normed = rms_scale(hidden, mix_gain)

    def project(weight):
        return jnp.dot(normed, weight, preferred_element_type=jnp.float32).astype(jnp.bfloat16)
    mixed, next_state = retain(project(query_weight), project(key_weight), project(value_weight), project(gate_weight), ret_state, positions, jnp.arange(HEADS, dtype=jnp.int32), head_gain)
    after = (hidden.astype(jnp.float32) + jnp.dot(mixed, out_weight, preferred_element_type=jnp.float32)).astype(jnp.bfloat16)
    inner = rms_scale(after, ffn_gain)
    pair_count = BATCH * TOP
    chosen = route_ids.reshape(pair_count).astype(jnp.int32)
    pair_rows = jnp.repeat(inner, TOP, axis=0)
    onehot = (chosen[:, None] == jnp.arange(EXPERTS, dtype=jnp.int32)[None, :]).astype(jnp.int32)
    ranks = lax.optimization_barrier(jnp.sum((jnp.cumsum(onehot, axis=0).astype(jnp.int32) - 1) * onehot, axis=1)).astype(jnp.int32)
    slots = jnp.arange(N_EP * CAP, dtype=jnp.int32)

    def one_expert(carry, index):
        select = ((chosen[None, :] == index) & (ranks[None, :] == slots[:, None])).astype(jnp.bfloat16)
        rows = jnp.dot(select, pair_rows, preferred_element_type=jnp.float32).astype(jnp.bfloat16)
        gate = jnp.dot(rows, expert_gate[index], preferred_element_type=jnp.float32)
        lifted = jnp.dot(rows, expert_up[index], preferred_element_type=jnp.float32)
        activated = (jax.nn.silu(gate) * lifted).astype(jnp.bfloat16)
        result = jnp.dot(activated, expert_down[index], preferred_element_type=jnp.float32).astype(jnp.bfloat16)
        return (carry + jnp.dot(select.T, result, preferred_element_type=jnp.float32), None)
    pair_out, unused = lax.scan(one_expert, jnp.zeros((pair_count, D), jnp.float32), jnp.arange(EXPERTS, dtype=jnp.int32))
    weighted = lax.optimization_barrier(jnp.sum(pair_out.reshape(BATCH, TOP, D) * route_weight[:, :, None], axis=1))
    updated = (after.astype(jnp.float32) + weighted).astype(jnp.bfloat16)
    return (updated, next_state)
```

```python
import functools

import jax
import jax.numpy as jnp
import numpy as np
from jax import lax
from jax.experimental import pallas as pl
from jax.experimental.pallas import tpu as pltpu
from jax.sharding import PartitionSpec as P

HEAD = 128
GROUPS = 4
TOP = 2
HEADS = 16
AUX = 128
epsilon = 1e-06
rope_base = 10000.0
MESH = pl.DeviceIdType.MESH
f32 = jnp.float32
bf16 = jnp.bfloat16


def thirds(x):
    hi = x.astype(bf16).astype(f32)
    mid = (x - hi).astype(bf16).astype(f32)
    return hi, mid, x - hi - mid


def dot(a, b):
    return jnp.dot(a, b, preferred_element_type=f32)


def kernel(c, hid, pos, inv, hgain, mgain, fgain, ids, rw, tab, perm, permt,
           wq, wk, wv, wg, wo_h, eg_h, eu_h, ed_h, st_h,
           out, nst_h,
           wqk, wo, wgu, wd, st, hg, nb, xb, pb, rb, qs, ks, vs, rd, ys, mg, xs, x1, ag, x2, acts, a2, yb, y1, y2,
           tsend, trecv, esend, erecv, lsem, osem):
    N, T, R, W, J, F = c.N, c.T, c.R, c.W, c.J, c.F
    Z = T // 2
    U, PU, SP, ME, cap = c.U, c.PU, c.SP, c.ME, c.cap
    heads, HW, D = c.heads, c.heads * HEAD, c.D
    e = lax.axis_index("ep")
    t = lax.axis_index("tp")
    z = t // 2
    core = t % 2
    sib = z * 2 + (1 - core)

    local = []

    def fetch(src, dst):
        cp = pltpu.make_async_copy(src, dst, lsem.at[len(local)])
        cp.start()
        local.append(cp)
        return cp

    proj_w = [fetch(w, wqk.at[:, pl.ds(n * HW, HW)]) for n, w in enumerate((wq, wk, wv, wg))]
    state_in = fetch(st_h, st)
    wo_in = fetch(wo_h, wo)
    gu_in = []
    for u in range(U):
        for i in range(PU):
            gu_in.append(fetch(eg_h.at[u * PU + i], wgu.at[u, :, pl.ds(2 * i * F, F)]))
            gu_in.append(fetch(eu_h.at[u * PU + i], wgu.at[u, :, pl.ds((2 * i + 1) * F, F)]))
    wd_in = fetch(ed_h, wd)

    barrier = pltpu.get_barrier_semaphore()
    for i in range(1, N):
        pl.semaphore_signal(barrier, inc=1, device_id=(lax.rem(e + i, N), t), device_id_type=MESH)
    for i in range(1, Z):
        pl.semaphore_signal(barrier, inc=1, device_id=(e, lax.rem(z + i, Z) * 2 + core), device_id_type=MESH)
    pl.semaphore_signal(barrier, inc=1, device_id=(e, sib), device_id_type=MESH)

    angle = pos[...].astype(f32) * inv[...]
    cosine = jnp.cos(angle)
    lane = lax.broadcasted_iota(jnp.int32, (R, HEAD), 1)
    sine = jnp.where(lane < HEAD // 2, -1.0, 1.0) * jnp.sin(angle)

    S = N * SP
    base = tab[0:1, :]
    want = tab[1:2, :]
    masks = [
        jnp.where((ids[:, k : k + 1] >= base) & (ids[:, k : k + 1] < base + PU), 1.0, 0.0) for k in range(TOP)
    ]
    member = functools.reduce(jnp.maximum, masks)
    row = lax.broadcasted_iota(jnp.int32, (R, R), 0)
    col = lax.broadcasted_iota(jnp.int32, (R, R), 1)
    lower = jnp.where(col < row, 1.0, 0.0).astype(bf16)
    rank = dot(lower, member.astype(bf16))
    hit = jnp.where(rank == want.astype(f32), 1.0, 0.0)
    place = member * hit
    place_t = jnp.transpose(place).astype(bf16)
    places_t = [jnp.transpose(m * hit).astype(bf16) for m in masks]
    lane_a = lax.broadcasted_iota(jnp.int32, (R, AUX), 1)
    aux_w = jnp.zeros((S, AUX), f32)
    for k in range(TOP):
        parts = thirds(rw[:, k : k + 1])
        which = (ids[:, k : k + 1] & (PU - 1)) * 3 + 3
        lanes = jnp.zeros((R, AUX), f32)
        for n in range(3):
            lanes = lanes + jnp.where(lane_a == which + n, parts[n], 0.0)
        aux_w = aux_w + dot(places_t[k], lanes.astype(bf16))

    pl.semaphore_wait(barrier, N - 1 + Z - 1 + 1)

    def tp_gather(ph, src, buf, use):
        sends = []

        def send(s, slot, peer, n):
            cp = pltpu.make_async_remote_copy(
                src_ref=s, dst_ref=buf.at[slot], send_sem=tsend.at[ph, n], recv_sem=trecv.at[ph, slot],
                device_id=(e, peer), device_id_type=MESH)
            cp.start()
            sends.append(cp)

        def arrive(slot, peer):
            pltpu.make_async_remote_copy(
                src_ref=src, dst_ref=buf.at[slot], send_sem=tsend.at[ph, 0], recv_sem=trecv.at[ph, slot],
                device_id=(e, peer), device_id_type=MESH).wait_recv()

        order = sorted(range(1, Z), key=lambda i: (min(i, Z - i), i))
        far = [lax.rem(z + i, Z) for i in order]
        for n, zz in enumerate(far):
            send(src, t, zz * 2 + core, n)
        send(src, t, sib, Z - 1)
        use(t, src)
        for n, zz in enumerate(far):
            slot = zz * 2 + core
            arrive(slot, slot)
            send(buf.at[slot], slot, sib, Z + n)
            if n == 0:
                arrive(sib, sib)
                use(sib, buf.at[sib])
            use(slot, buf.at[slot])
        for n, zz in enumerate(far):
            slot = zz * 2 + (1 - core)
            arrive(slot, sib)
            use(slot, buf.at[slot])
        return sends

    def ep_send(ph, i, src, buf):
        cp = pltpu.make_async_remote_copy(
            src_ref=src, dst_ref=buf.at[e], send_sem=esend.at[ph, i], recv_sem=erecv.at[ph, e],
            device_id=(lax.rem(e + i, N), t), device_id_type=MESH)
        cp.start()
        return cp

    def ep_arrive(ph, i, buf):
        peer = lax.rem(e + i, N)
        pltpu.make_async_remote_copy(
            src_ref=buf.at[peer], dst_ref=buf.at[peer], send_sem=esend.at[ph, i], recv_sem=erecv.at[ph, peer],
            device_id=(peer, t), device_id_type=MESH).wait_recv()

    done = []

    hbox = [jnp.zeros((R, W), f32)]

    def square(slot, ref):
        v = ref[...].astype(f32)
        hbox[0] = hbox[0] + v * v

    done += tp_gather(0, hid, hg, square)
    hg[t] = hid[...]
    factor = lax.rsqrt(jnp.sum(hbox[0], axis=1, keepdims=True) / D + epsilon)

    def norm_block(slot):
        g = mgain[:, pl.ds(pl.multiple_of(slot * W, W), W)]
        return (hg[slot].astype(f32) * factor * g).astype(bf16)

    for i in range(1, N):
        peer = lax.rem(e + i, N)
        for j in range(J):
            nb[peer, j] = norm_block(peer * J + j)
        done.append(ep_send(0, i, nb.at[peer], xb))
    for j in range(J):
        nb[e, j] = norm_block(e * J + j)

    for cp in proj_w:
        cp.wait()

    def project(ref, slot):
        return sum(dot(ref[slot, j], wqk[j * W : (j + 1) * W, :]) for j in range(J))

    total = project(nb, e)
    for i in range(1, N):
        ep_arrive(0, i, xb)
        peer = lax.rem(e + i, N)
        pb[peer] = project(xb, peer).astype(bf16)
        done.append(ep_send(1, i, pb.at[peer], rb))
    for i in range(1, N):
        ep_arrive(1, i, rb)
        total = total + rb[lax.rem(e + i, N)].astype(f32)
    total = total.astype(bf16).astype(f32)

    vs[...] = total[:, 2 * HW : 3 * HW]
    for h in range(heads):
        at = slice(h * HEAD, (h + 1) * HEAD)
        q = total[:, h * HEAD : (h + 1) * HEAD]
        k = total[:, HW + h * HEAD : HW + (h + 1) * HEAD]
        qs[:, at] = q * cosine + pltpu.roll(q, HEAD // 2, 1) * sine
        ks[:, at] = (k * cosine + pltpu.roll(k, HEAD // 2, 1) * sine) * HEAD ** (-0.5)
    decays = []
    for h in range(heads):
        number = (jnp.zeros((1, HEAD), jnp.int32) + (t * heads + h)).astype(f32)
        decays.append(1.0 - jnp.exp2(-5.0 - 5.0 * number / (HEADS - 1)))
    state_in.wait()

    def group(g, carry):
        rows = pl.ds(pl.multiple_of(g * 8, 8), 8)
        for h in range(heads):
            at = slice(h * HEAD, (h + 1) * HEAD)
            qt = jnp.transpose(qs[rows, at])
            kt = jnp.transpose(ks[rows, at])
            v8 = vs[rows, at]
            reads = []
            for b in range(8):
                new = decays[h] * st[g * 8 + b, h] + kt[:, b : b + 1] * v8[b : b + 1, :]
                st[g * 8 + b, h] = new
                reads.append(jnp.sum(qt[:, b : b + 1] * new, axis=0, keepdims=True))
            rd[rows, at] = jnp.concatenate(reads, axis=0)
        return carry

    lax.fori_loop(0, R // 8, group, 0)
    state_out = pltpu.make_async_copy(st, nst_h, osem)
    state_out.start()

    for h in range(heads):
        at = slice(h * HEAD, (h + 1) * HEAD)
        read = rd[:, at]
        centered = read - jnp.mean(read, axis=1, keepdims=True)
        normal = centered * lax.rsqrt(jnp.mean(centered * centered, axis=1, keepdims=True) + epsilon)
        gate = total[:, 3 * HW + h * HEAD : 3 * HW + (h + 1) * HEAD]
        ys[:, at] = (normal * hgain[:, at] * (gate * jax.nn.sigmoid(gate))).astype(bf16)

    wo_in.wait()
    pbox = [jnp.zeros((R, W), f32)]

    def out_project(slot, ref):
        w = wo[pl.ds(pl.multiple_of(slot * HW, HW), HW), :]
        pbox[0] = pbox[0] + dot(ref[...], w)

    done += tp_gather(1, ys, mg, out_project)
    after = (hid[...].astype(f32) + pbox[0]).astype(bf16).astype(f32)

    squares = thirds(jnp.sum(after * after, axis=1, keepdims=True))
    lanes = jnp.zeros((R, AUX), f32)
    for n in range(3):
        lanes = lanes + jnp.where(lane_a == n, squares[n], 0.0)
    gained = (after * fgain[:, pl.ds(pl.multiple_of(t * W, W), W)]).astype(bf16)
    packed = dot(place_t, gained).astype(bf16)
    packed_aux = (dot(place_t, lanes.astype(bf16)) + aux_w).astype(bf16)
    for n in range(N):
        xs[n, :, 0:W] = packed[n * SP : (n + 1) * SP, :]
        xs[n, :, W:] = packed_aux[n * SP : (n + 1) * SP, :]
    for i in range(1, N):
        done.append(ep_send(2, i, xs.at[lax.rem(e + i, N)], x1))
    x1[e] = xs[e]
    for i in range(1, N):
        ep_arrive(2, i, x1)
    own = dot(perm[...], x1[...].reshape(S, W + AUX)).astype(bf16)
    ag[...] = own
    weight_aux = own[:, W:].astype(f32)
    for cp in gu_in:
        cp.wait()
    MU = ME // U
    fbox = [jnp.zeros((ME, AUX), f32)] + [jnp.zeros((MU, PU * 2 * F), f32) for u in range(U)]

    def first(slot, ref):
        fbox[0] = fbox[0] + ref[:, W:].astype(f32)
        at = pl.ds(pl.multiple_of(slot * W, W), W)
        for u in range(U):
            fbox[1 + u] = fbox[1 + u] + dot(ref[u * MU : (u + 1) * MU, 0:W], wgu[u, at, :])

    done += tp_gather(2, ag, x2, first)
    sq = fbox[0][:, 0:1] + fbox[0][:, 1:2] + fbox[0][:, 2:3]
    scale = lax.rsqrt(sq / D + epsilon)
    for u in range(U):
        both = fbox[1 + u] * scale[u * MU : (u + 1) * MU, :]
        for i in range(PU):
            gate = both[:, 2 * i * F : (2 * i + 1) * F]
            lifted = both[:, (2 * i + 1) * F : (2 * i + 2) * F]
            acts[u * MU : (u + 1) * MU, i * F : (i + 1) * F] = (gate * jax.nn.sigmoid(gate) * lifted).astype(bf16)

    wd_in.wait()
    dbox = [jnp.zeros((MU, W), f32) for _ in range(U * PU)]

    def second(slot, ref):
        at = pl.ds(pl.multiple_of(slot * F, F), F)
        for u in range(U):
            for i in range(PU):
                n = u * PU + i
                dbox[n] = dbox[n] + dot(ref[u * MU : (u + 1) * MU, i * F : (i + 1) * F], wd[n, at, :])

    done += tp_gather(3, acts, a2, second)
    for u in range(U):
        mixture = jnp.zeros((MU, W), f32)
        for i in range(PU):
            three = weight_aux[u * MU : (u + 1) * MU, 3 + 3 * i : 6 + 3 * i]
            mixture = mixture + dbox[u * PU + i] * (three[:, 0:1] + three[:, 1:2] + three[:, 2:3])
        yb[u * MU : (u + 1) * MU, :] = mixture.astype(bf16)
    y1[...] = dot(permt[...], yb[...]).astype(bf16).reshape(N, SP, W)
    for i in range(1, N):
        done.append(ep_send(3, i, y1.at[lax.rem(e + i, N)], y2))
    y2[e] = y1[e]
    for i in range(1, N):
        ep_arrive(3, i, y2)
    out[...] = (after + dot(place.astype(bf16), y2[...].reshape(S, W))).astype(bf16)

    for cp in done:
        cp.wait_send()
    state_out.wait()


class Sizes:
    pass


def per_device(hidden, positions, ret_state, query_weight, key_weight, value_weight, gate_weight, head_gain,
               out_weight, mix_gain, ffn_gain, expert_gate, expert_up, expert_down, route_ids, route_weight):
    c = Sizes()
    c.N = N = lax.axis_size("ep")
    c.T = T = lax.axis_size("tp")
    c.R, c.W = R, W = hidden.shape
    c.D = D = mix_gain.shape[0]
    c.J = J = query_weight.shape[0] // W
    c.F = F = expert_gate.shape[2]
    c.heads = heads = query_weight.shape[1] // HEAD
    HW = heads * HEAD
    local_experts = expert_gate.shape[0]
    group_size = local_experts * N // GROUPS
    c.cap = cap = 2 * ((R // GROUPS + group_size - 1) // group_size)
    c.PU = PU = TOP if group_size == TOP and local_experts % TOP == 0 else 1
    c.U = U = local_experts // PU
    c.SP = SP = (U * cap + 15) // 16 * 16
    c.ME = ME = U * N * cap
    S = N * SP
    assert J * W * N == D and T % 2 == 0 and R % 8 == 0

    tab = np.full((2, S), -1000, np.int32)
    perm = np.zeros((ME, S), np.float32)
    for n in range(N):
        for u in range(U):
            for r in range(cap):
                s = n * SP + u * cap + r
                tab[0, s] = (n * U + u) * PU
                tab[1, s] = r
                perm[(u * N + n) * cap + r, s] = 1.0
    half = np.arange(0, HEAD, 2, dtype=np.float32) / HEAD
    inv = (1.0 / rope_base ** half.astype(np.float64)).astype(np.float32)
    inv = np.concatenate([inv, inv])[None, :]

    V = pl.BlockSpec(memory_space=pltpu.VMEM)
    A = pl.BlockSpec(memory_space=pl.ANY)
    names = [
        ((D // N, 4 * HW), bf16),
        ((T * HW, W), bf16),
        ((U, D, PU * 2 * F), bf16),
        (expert_down.shape, bf16),
        (ret_state.shape, f32),
        ((T, R, W), bf16),
        ((N, J, R, W), bf16),
        ((N, J, R, W), bf16),
        ((N, R, 4 * HW), bf16),
        ((N, R, 4 * HW), bf16),
        ((R, HW), f32),
        ((R, HW), f32),
        ((R, HW), f32),
        ((R, HW), f32),
        ((R, HW), bf16),
        ((T, R, HW), bf16),
        ((N, SP, W + AUX), bf16),
        ((N, SP, W + AUX), bf16),
        ((ME, W + AUX), bf16),
        ((T, ME, W + AUX), bf16),
        ((ME, PU * F), bf16),
        ((T, ME, PU * F), bf16),
        ((ME, W), bf16),
        ((N, SP, W), bf16),
        ((N, SP, W), bf16),
    ]
    updated, next_state = pl.pallas_call(
        functools.partial(kernel, c),
        out_shape=(jax.ShapeDtypeStruct((R, W), bf16), jax.ShapeDtypeStruct(ret_state.shape, f32)),
        in_specs=[V] * 11 + [A] * 9,
        out_specs=(V, A),
        scratch_shapes=[pltpu.VMEM(shape, kind) for shape, kind in names] + [
            pltpu.SemaphoreType.DMA((4, T)),
            pltpu.SemaphoreType.DMA((4, T)),
            pltpu.SemaphoreType.DMA((4, N)),
            pltpu.SemaphoreType.DMA((4, N)),
            pltpu.SemaphoreType.DMA((7 + 2 * local_experts,)),
            pltpu.SemaphoreType.DMA,
        ],
        compiler_params=pltpu.CompilerParams(
            collective_id=0, has_side_effects=True, vmem_limit_bytes=48 * 1024 * 1024
        ),
    )(hidden, positions.reshape(R, 1), jnp.asarray(inv), head_gain.reshape(1, HW), mix_gain.reshape(1, D),
      ffn_gain.reshape(1, D), route_ids, route_weight, jnp.asarray(tab), jnp.asarray(perm, bf16),
      jnp.asarray(perm.T, bf16),
      query_weight, key_weight, value_weight, gate_weight, out_weight, expert_gate, expert_up, expert_down, ret_state)
    return updated, next_state


def solution(mesh):
    return jax.shard_map(
        per_device,
        mesh=mesh,
        in_specs=(
            P("ep", "tp"), P("ep"), P("ep", "tp", None, None),
            P("ep", "tp"), P("ep", "tp"), P("ep", "tp"), P("ep", "tp"),
            P("tp"), P(None, "tp"), P(), P(),
            P("ep", None, "tp"), P("ep", None, "tp"), P("ep", None, "tp"),
            P("ep", None), P("ep", None),
        ),
        out_specs=(P("ep", "tp"), P("ep", "tp", None, None)),
        check_vma=False,
    )
```

```python
import functools

import jax
import jax.numpy as jnp
import numpy as np
from jax import lax
from jax.experimental import pallas as pl
from jax.experimental.pallas import tpu as pltpu
from jax.sharding import PartitionSpec as P

HEAD = 128
GROUPS = 4
TOP = 2
HEADS = 16
AUX = 128
epsilon = 1e-06
rope_base = 10000.0
MESH = pl.DeviceIdType.MESH
f32 = jnp.float32
bf16 = jnp.bfloat16


def thirds(x):
    hi = x.astype(bf16).astype(f32)
    mid = (x - hi).astype(bf16).astype(f32)
    return hi, mid, x - hi - mid


def dot(a, b):
    return jnp.dot(a, b, preferred_element_type=f32)


def kernel(c, hid_h, pos_h, inv_h, hgain_h, mgain_h, fgain_h, ids_h, rw_h, tab_h, perm_h, permt_h,
           wq, wk, wv, wg, wo_h, eg_h, eu_h, ed_h, st_h,
           out, st,
           hid, pos, inv, hgain, mgain, fgain, idr, rwr, tab, perm, permt,
           wqk, wo, wgu, wd, hg, nb, xb, pb, rb, qs, ks, vs, rd, ys, mg, xs, x1, ag, x2, acts, a2, yb, y1, y2,
           tsend, trecv, esend, erecv, lsem):
    N, T, R, W, J, F = c.N, c.T, c.R, c.W, c.J, c.F
    Z = T // 2
    U, PU, SP, ME, cap = c.U, c.PU, c.SP, c.ME, c.cap
    heads, HW, D = c.heads, c.heads * HEAD, c.D
    e = lax.axis_index("ep")
    t = lax.axis_index("tp")
    z = t // 2
    core = t % 2
    sib = z * 2 + (1 - core)

    local = []

    def fetch(src, dst):
        cp = pltpu.make_async_copy(src, dst, lsem.at[len(local)])
        cp.start()
        local.append(cp)
        return cp

    hid_in = fetch(hid_h, hid)
    small = [fetch(a, b) for a, b in (
        (pos_h, pos), (inv_h, inv), (hgain_h, hgain), (mgain_h, mgain), (fgain_h, fgain), (ids_h, idr), (rw_h, rwr),
        (tab_h, tab), (perm_h, perm), (permt_h, permt))]
    proj_w = [fetch(w, wqk.at[:, pl.ds(n * HW, HW)]) for n, w in enumerate((wq, wk, wv, wg))]
    state_in = fetch(st_h, st)
    wo_in = fetch(wo_h, wo)
    gu_in = []
    for u in range(U):
        for i in range(PU):
            gu_in.append(fetch(eg_h.at[u * PU + i], wgu.at[u, :, pl.ds(2 * i * F, F)]))
            gu_in.append(fetch(eu_h.at[u * PU + i], wgu.at[u, :, pl.ds((2 * i + 1) * F, F)]))
    wd_in = fetch(ed_h, wd)

    barrier = pltpu.get_barrier_semaphore()
    for i in range(1, N):
        pl.semaphore_signal(barrier, inc=1, device_id=(lax.rem(e + i, N), t), device_id_type=MESH)
    for i in range(1, Z):
        pl.semaphore_signal(barrier, inc=1, device_id=(e, lax.rem(z + i, Z) * 2 + core), device_id_type=MESH)
    pl.semaphore_signal(barrier, inc=1, device_id=(e, sib), device_id_type=MESH)

    for cp in small:
        cp.wait()
    row = lax.broadcasted_iota(jnp.int32, (R, R), 0)
    col = lax.broadcasted_iota(jnp.int32, (R, R), 1)

    def stand(line):
        return jnp.sum(jnp.where(row == col, line, 0.0), axis=1, keepdims=True)

    ids = [stand(idr[k : k + 1, :].astype(f32)).astype(jnp.int32) for k in range(TOP)]
    rw = [stand(rwr[k : k + 1, :]) for k in range(TOP)]
    angle = stand(pos[...].astype(f32)) * inv[...]
    cosine = jnp.cos(angle)
    lane = lax.broadcasted_iota(jnp.int32, (R, HEAD), 1)
    sine = jnp.where(lane < HEAD // 2, -1.0, 1.0) * jnp.sin(angle)

    S = N * SP
    base = tab[0:1, :]
    want = tab[1:2, :]
    masks = [
        jnp.where((ids[k] >= base) & (ids[k] < base + PU), 1.0, 0.0) for k in range(TOP)
    ]
    member = functools.reduce(jnp.maximum, masks)
    lower = jnp.where(col < row, 1.0, 0.0).astype(bf16)
    rank = dot(lower, member.astype(bf16))
    hit = jnp.where(rank == want.astype(f32), 1.0, 0.0)
    place = member * hit
    place_t = jnp.transpose(place).astype(bf16)
    places_t = [jnp.transpose(m * hit).astype(bf16) for m in masks]
    lane_a = lax.broadcasted_iota(jnp.int32, (R, AUX), 1)
    aux_w = jnp.zeros((S, AUX), f32)
    for k in range(TOP):
        parts = thirds(rw[k])
        which = (ids[k] & (PU - 1)) * 3 + 3
        lanes = jnp.zeros((R, AUX), f32)
        for n in range(3):
            lanes = lanes + jnp.where(lane_a == which + n, parts[n], 0.0)
        aux_w = aux_w + dot(places_t[k], lanes.astype(bf16))

    hid_in.wait()
    pl.semaphore_wait(barrier, N - 1 + Z - 1 + 1)

    def tp_gather(ph, src, buf, use):
        sends = []

        def send(s, slot, peer, n):
            cp = pltpu.make_async_remote_copy(
                src_ref=s, dst_ref=buf.at[slot], send_sem=tsend.at[ph, n], recv_sem=trecv.at[ph, slot],
                device_id=(e, peer), device_id_type=MESH)
            cp.start()
            sends.append(cp)

        def arrive(slot, peer):
            pltpu.make_async_remote_copy(
                src_ref=src, dst_ref=buf.at[slot], send_sem=tsend.at[ph, 0], recv_sem=trecv.at[ph, slot],
                device_id=(e, peer), device_id_type=MESH).wait_recv()

        order = sorted(range(1, Z), key=lambda i: (min(i, Z - i), i))
        far = [lax.rem(z + i, Z) for i in order]
        for n, zz in enumerate(far):
            send(src, t, zz * 2 + core, n)
        send(src, t, sib, Z - 1)
        use(t, src)
        for n, zz in enumerate(far):
            slot = zz * 2 + core
            arrive(slot, slot)
            send(buf.at[slot], slot, sib, Z + n)
            if n == 0:
                arrive(sib, sib)
                use(sib, buf.at[sib])
            use(slot, buf.at[slot])
        for n, zz in enumerate(far):
            slot = zz * 2 + (1 - core)
            arrive(slot, sib)
            use(slot, buf.at[slot])
        return sends

    def ep_send(ph, i, src, buf):
        cp = pltpu.make_async_remote_copy(
            src_ref=src, dst_ref=buf.at[e], send_sem=esend.at[ph, i], recv_sem=erecv.at[ph, e],
            device_id=(lax.rem(e + i, N), t), device_id_type=MESH)
        cp.start()
        return cp

    def ep_arrive(ph, i, buf):
        peer = lax.rem(e + i, N)
        pltpu.make_async_remote_copy(
            src_ref=buf.at[peer], dst_ref=buf.at[peer], send_sem=esend.at[ph, i], recv_sem=erecv.at[ph, peer],
            device_id=(peer, t), device_id_type=MESH).wait_recv()

    done = []

    hbox = [jnp.zeros((R, W), f32)]

    def square(slot, ref):
        v = ref[...].astype(f32)
        hbox[0] = hbox[0] + v * v

    done += tp_gather(0, hid, hg, square)
    hg[t] = hid[...]
    factor = lax.rsqrt(jnp.sum(hbox[0], axis=1, keepdims=True) / D + epsilon)

    def norm_block(slot):
        g = mgain[:, pl.ds(pl.multiple_of(slot * W, W), W)]
        return (hg[slot].astype(f32) * factor * g).astype(bf16)

    for i in range(1, N):
        peer = lax.rem(e + i, N)
        for j in range(J):
            nb[peer, j] = norm_block(peer * J + j)
        done.append(ep_send(0, i, nb.at[peer], xb))
    for j in range(J):
        nb[e, j] = norm_block(e * J + j)

    for cp in proj_w:
        cp.wait()

    def project(ref, slot):
        return sum(dot(ref[slot, j], wqk[j * W : (j + 1) * W, :]) for j in range(J))

    total = project(nb, e)
    for i in range(1, N):
        ep_arrive(0, i, xb)
        peer = lax.rem(e + i, N)
        pb[peer] = project(xb, peer).astype(bf16)
        done.append(ep_send(1, i, pb.at[peer], rb))
    for i in range(1, N):
        ep_arrive(1, i, rb)
        total = total + rb[lax.rem(e + i, N)].astype(f32)
    total = total.astype(bf16).astype(f32)

    vs[...] = total[:, 2 * HW : 3 * HW]
    for h in range(heads):
        at = slice(h * HEAD, (h + 1) * HEAD)
        q = total[:, h * HEAD : (h + 1) * HEAD]
        k = total[:, HW + h * HEAD : HW + (h + 1) * HEAD]
        qs[:, at] = q * cosine + pltpu.roll(q, HEAD // 2, 1) * sine
        ks[:, at] = (k * cosine + pltpu.roll(k, HEAD // 2, 1) * sine) * HEAD ** (-0.5)
    decays = []
    for h in range(heads):
        number = (jnp.zeros((1, HEAD), jnp.int32) + (t * heads + h)).astype(f32)
        decays.append(1.0 - jnp.exp2(-5.0 - 5.0 * number / (HEADS - 1)))
    state_in.wait()

    def group(g, carry):
        rows = pl.ds(pl.multiple_of(g * 8, 8), 8)
        for h in range(heads):
            at = slice(h * HEAD, (h + 1) * HEAD)
            qt = jnp.transpose(qs[rows, at])
            kt = jnp.transpose(ks[rows, at])
            v8 = vs[rows, at]
            reads = []
            for b in range(8):
                new = decays[h] * st[g * 8 + b, h] + kt[:, b : b + 1] * v8[b : b + 1, :]
                st[g * 8 + b, h] = new
                reads.append(jnp.sum(qt[:, b : b + 1] * new, axis=0, keepdims=True))
            rd[rows, at] = jnp.concatenate(reads, axis=0)
        return carry

    lax.fori_loop(0, R // 8, group, 0)

    for h in range(heads):
        at = slice(h * HEAD, (h + 1) * HEAD)
        read = rd[:, at]
        centered = read - jnp.mean(read, axis=1, keepdims=True)
        normal = centered * lax.rsqrt(jnp.mean(centered * centered, axis=1, keepdims=True) + epsilon)
        gate = total[:, 3 * HW + h * HEAD : 3 * HW + (h + 1) * HEAD]
        ys[:, at] = (normal * hgain[:, at] * (gate * jax.nn.sigmoid(gate))).astype(bf16)

    wo_in.wait()
    pbox = [jnp.zeros((R, W), f32)]

    def out_project(slot, ref):
        w = wo[pl.ds(pl.multiple_of(slot * HW, HW), HW), :]
        pbox[0] = pbox[0] + dot(ref[...], w)

    done += tp_gather(1, ys, mg, out_project)
    after = (hid[...].astype(f32) + pbox[0]).astype(bf16).astype(f32)

    squares = thirds(jnp.sum(after * after, axis=1, keepdims=True))
    lanes = jnp.zeros((R, AUX), f32)
    for n in range(3):
        lanes = lanes + jnp.where(lane_a == n, squares[n], 0.0)
    gained = (after * fgain[:, pl.ds(pl.multiple_of(t * W, W), W)]).astype(bf16)
    packed = dot(place_t, gained).astype(bf16)
    packed_aux = (dot(place_t, lanes.astype(bf16)) + aux_w).astype(bf16)
    for n in range(N):
        xs[n, :, 0:W] = packed[n * SP : (n + 1) * SP, :]
        xs[n, :, W:] = packed_aux[n * SP : (n + 1) * SP, :]
    for i in range(1, N):
        done.append(ep_send(2, i, xs.at[lax.rem(e + i, N)], x1))
    x1[e] = xs[e]
    for i in range(1, N):
        ep_arrive(2, i, x1)
    own = dot(perm[...], x1[...].reshape(S, W + AUX)).astype(bf16)
    ag[...] = own
    weight_aux = own[:, W:].astype(f32)
    for cp in gu_in:
        cp.wait()
    MU = ME // U
    fbox = [jnp.zeros((ME, AUX), f32)] + [jnp.zeros((MU, PU * 2 * F), f32) for u in range(U)]

    def first(slot, ref):
        fbox[0] = fbox[0] + ref[:, W:].astype(f32)
        at = pl.ds(pl.multiple_of(slot * W, W), W)
        for u in range(U):
            fbox[1 + u] = fbox[1 + u] + dot(ref[u * MU : (u + 1) * MU, 0:W], wgu[u, at, :])

    done += tp_gather(2, ag, x2, first)
    sq = fbox[0][:, 0:1] + fbox[0][:, 1:2] + fbox[0][:, 2:3]
    scale = lax.rsqrt(sq / D + epsilon)
    for u in range(U):
        both = fbox[1 + u] * scale[u * MU : (u + 1) * MU, :]
        for i in range(PU):
            gate = both[:, 2 * i * F : (2 * i + 1) * F]
            lifted = both[:, (2 * i + 1) * F : (2 * i + 2) * F]
            acts[u * MU : (u + 1) * MU, i * F : (i + 1) * F] = (gate * jax.nn.sigmoid(gate) * lifted).astype(bf16)

    wd_in.wait()
    dbox = [jnp.zeros((MU, W), f32) for _ in range(U * PU)]

    def second(slot, ref):
        at = pl.ds(pl.multiple_of(slot * F, F), F)
        for u in range(U):
            for i in range(PU):
                n = u * PU + i
                dbox[n] = dbox[n] + dot(ref[u * MU : (u + 1) * MU, i * F : (i + 1) * F], wd[n, at, :])

    done += tp_gather(3, acts, a2, second)
    for u in range(U):
        mixture = jnp.zeros((MU, W), f32)
        for i in range(PU):
            three = weight_aux[u * MU : (u + 1) * MU, 3 + 3 * i : 6 + 3 * i]
            mixture = mixture + dbox[u * PU + i] * (three[:, 0:1] + three[:, 1:2] + three[:, 2:3])
        yb[u * MU : (u + 1) * MU, :] = mixture.astype(bf16)
    y1[...] = dot(permt[...], yb[...]).astype(bf16).reshape(N, SP, W)
    for i in range(1, N):
        done.append(ep_send(3, i, y1.at[lax.rem(e + i, N)], y2))
    y2[e] = y1[e]
    for i in range(1, N):
        ep_arrive(3, i, y2)
    out[...] = (after + dot(place.astype(bf16), y2[...].reshape(S, W))).astype(bf16)

    for cp in done:
        cp.wait_send()


class Sizes:
    pass


def per_device(hidden, positions, ret_state, query_weight, key_weight, value_weight, gate_weight, head_gain,
               out_weight, mix_gain, ffn_gain, expert_gate, expert_up, expert_down, route_ids, route_weight):
    c = Sizes()
    c.N = N = lax.axis_size("ep")
    c.T = T = lax.axis_size("tp")
    c.R, c.W = R, W = hidden.shape
    c.D = D = mix_gain.shape[0]
    c.J = J = query_weight.shape[0] // W
    c.F = F = expert_gate.shape[2]
    c.heads = heads = query_weight.shape[1] // HEAD
    HW = heads * HEAD
    local_experts = expert_gate.shape[0]
    group_size = local_experts * N // GROUPS
    c.cap = cap = 2 * ((R // GROUPS + group_size - 1) // group_size)
    c.PU = PU = TOP if group_size == TOP and local_experts % TOP == 0 else 1
    c.U = U = local_experts // PU
    c.SP = SP = (U * cap + 15) // 16 * 16
    c.ME = ME = U * N * cap
    S = N * SP
    assert J * W * N == D and T % 2 == 0 and R % 8 == 0

    tab = np.full((2, S), -1000, np.int32)
    perm = np.zeros((ME, S), np.float32)
    for n in range(N):
        for u in range(U):
            for r in range(cap):
                s = n * SP + u * cap + r
                tab[0, s] = (n * U + u) * PU
                tab[1, s] = r
                perm[(u * N + n) * cap + r, s] = 1.0
    half = np.arange(0, HEAD, 2, dtype=np.float32) / HEAD
    inv = (1.0 / rope_base ** half.astype(np.float64)).astype(np.float32)
    inv = np.concatenate([inv, inv])[None, :]

    V = pl.BlockSpec(memory_space=pltpu.VMEM)
    A = pl.BlockSpec(memory_space=pltpu.HBM)
    names = [
        ((R, W), bf16),
        ((1, R), jnp.int32),
        ((1, HEAD), f32),
        ((1, HW), f32),
        ((1, D), f32),
        ((1, D), f32),
        ((TOP, R), jnp.int32),
        ((TOP, R), f32),
        ((2, S), jnp.int32),
        ((ME, S), bf16),
        ((S, ME), bf16),
        ((D // N, 4 * HW), bf16),
        ((T * HW, W), bf16),
        ((U, D, PU * 2 * F), bf16),
        (expert_down.shape, bf16),
        ((T, R, W), bf16),
        ((N, J, R, W), bf16),
        ((N, J, R, W), bf16),
        ((N, R, 4 * HW), bf16),
        ((N, R, 4 * HW), bf16),
        ((R, HW), f32),
        ((R, HW), f32),
        ((R, HW), f32),
        ((R, HW), f32),
        ((R, HW), bf16),
        ((T, R, HW), bf16),
        ((N, SP, W + AUX), bf16),
        ((N, SP, W + AUX), bf16),
        ((ME, W + AUX), bf16),
        ((T, ME, W + AUX), bf16),
        ((ME, PU * F), bf16),
        ((T, ME, PU * F), bf16),
        ((ME, W), bf16),
        ((N, SP, W), bf16),
        ((N, SP, W), bf16),
    ]
    updated, next_state = pl.pallas_call(
        functools.partial(kernel, c),
        out_shape=(pltpu.VMEM((R, W), bf16), pltpu.VMEM(ret_state.shape, f32)),
        in_specs=[A] * 20,
        out_specs=(V, V),
        scratch_shapes=[pltpu.VMEM(shape, kind) for shape, kind in names] + [
            pltpu.SemaphoreType.DMA((4, T)),
            pltpu.SemaphoreType.DMA((4, T)),
            pltpu.SemaphoreType.DMA((4, N)),
            pltpu.SemaphoreType.DMA((4, N)),
            pltpu.SemaphoreType.DMA((18 + 2 * local_experts,)),
        ],
        compiler_params=pltpu.CompilerParams(
            collective_id=0, has_side_effects=True, vmem_limit_bytes=56 * 1024 * 1024
        ),
    )(*(pltpu.with_memory_space_constraint(x, pltpu.HBM) for x in (hidden, positions.reshape(1, R), jnp.asarray(inv), head_gain.reshape(1, HW), mix_gain.reshape(1, D),
      ffn_gain.reshape(1, D), route_ids.T, route_weight.T, jnp.asarray(tab), jnp.asarray(perm, bf16),
      jnp.asarray(perm.T, bf16),
      query_weight, key_weight, value_weight, gate_weight, out_weight, expert_gate, expert_up, expert_down, ret_state)))
    return updated, next_state


def solution(mesh):
    return jax.shard_map(
        per_device,
        mesh=mesh,
        in_specs=(
            P("ep", "tp"), P("ep"), P("ep", "tp", None, None),
            P("ep", "tp"), P("ep", "tp"), P("ep", "tp"), P("ep", "tp"),
            P("tp"), P(None, "tp"), P(), P(),
            P("ep", None, "tp"), P("ep", None, "tp"), P("ep", None, "tp"),
            P("ep", None), P("ep", None),
        ),
        out_specs=(P("ep", "tp"), P("ep", "tp", None, None)),
        check_vma=False,
    )
```
